32 devices in a mesh: rep: 2 (over x), fs: 8 (over z, y), tp: 2 (over core).
Axes of the slice: x: 2, y: 2, z: 4, core: 2. Of those that a mesh axis runs over, the one named last changes fastest.
Arguments:
- tokens: bfloat16 [5120, 2048], P(('rep', 'fs')), may hold values from -6 to 6
- gate_weight: float32 [2048, 5120], P('fs', 'tp'), may hold values from -0.125 to 0.125
- up_weight: float32 [2048, 5120], P('fs', 'tp'), may hold values from -0.125 to 0.125
- down_weight: float32 [2048, 5120], P('fs', 'tp'), may hold values from -0.078125 to 0.078125
- value_weight: float32 [2048, 2048], P('fs', 'tp'), may hold values from -0.125 to 0.125
- glu_weight: float32 [2048, 2048], P('fs', 'tp'), may hold values from -0.125 to 0.125
- out_weight: float32 [2048, 2048], P('fs', 'tp'), may hold values from -0.125 to 0.125
- gate_scale: float32 [5120], P('tp'), may hold values from 0.1 to 1.9
- up_scale: float32 [5120], P('tp'), may hold values from 0.5 to 2
- down_scale: float32 [2048], P('fs'), may hold values from 1 to 4
- value_scale: float32 [2048], P('tp'), may hold values from 0.2 to 3.4
- glu_scale: float32 [2048], P('tp'), may hold values from 0.1 to 1.9
- out_scale: float32 [2048], P('fs'), may hold values from 1 to 4
- conv_kernel: float32 [31, 2048], P(None, 'tp'), may hold values from -1 to 1
- norm_gain: float32 [2048], P('tp'), may hold values from 0.1 to 1.9
- first_gain: float32 [2048], replicated, may hold values from 0.1 to 1.9
- conv_gain: float32 [2048], replicated, may hold values from 0.1 to 1.9
- second_gain: float32 [2048], replicated, may hold values from 0.1 to 1.9
Outputs:
- result: bfloat16 [5120, 2048], P(('rep', 'fs'))
The draws below stay inside these ranges and needn't reach their ends.
All inputs are finite; a program needn't handle non-finite values.
Results may differ from the reference program's by a relative error of at most 0.02.
Values may be sent and summed in bfloat16 or wider, within the bound.
A program may use at most 128 MiB of HBM per device.

```python
import math
import jax
import jax.numpy as jnp
from jax import lax

D = 2048
FF = 5120
KW = 31
SEQ = 320
TOKENS = 5120
N_REP = 2
N_FS = 8
N_TP = 2


def draw_value_scale(key, part):
    position = jnp.arange(D, dtype=jnp.float32) / D
    noise = jax.random.uniform(key, (D,), jnp.float32, 0.7, 1.4)
    ramp = 0.5 * jnp.exp(jnp.log(4.0) * position)
    return (ramp * noise).astype(jnp.float32)


def shard_levels(rng, shape, pieces, least, high):
    level, own = 1.0, jax.random.fold_in(rng, 6)
    for dim, blocks in pieces:
        draws = jnp.exp(jax.random.uniform(jax.random.fold_in(own, dim), (blocks,), jnp.float32, least / len(pieces), high / len(pieces)))
        level = level * jnp.repeat(draws, shape[dim] // blocks).reshape([-1 if axis == dim else 1 for axis in range(len(shape))])
    return level


def scatter_about(own_key, extent, scale, most, shards=(), kind=jnp.bfloat16):
    array = jax.random.normal(own_key, extent, jnp.float32) * scale
    if len(shards) > 0:
        array = shard_levels(own_key, extent, shards, -0.22, 0.18) * array
    return jnp.clip(array, min=-most, max=most).astype(kind)


def setup_inputs(seed: int = 0) -> dict:
    key_of = jax.random.split(jax.random.key(seed), 19)
    return {
        "tokens": scatter_about(key_of[0], (TOKENS, D), 1.0, 6.0, ((0, 16),)),
        "gate_weight": scatter_about(key_of[1], (D, FF), D ** -0.5, 0.125, ((0, 8), (1, 2)), jnp.float32),
        "up_weight": scatter_about(key_of[2], (D, FF), D ** -0.5, 0.125, ((0, 8), (1, 2)), jnp.float32),
        "down_weight": scatter_about(key_of[3], (D, FF), FF ** -0.5, 0.078125, ((0, 8), (1, 2)), jnp.float32),
        "value_weight": scatter_about(key_of[4], (D, D), D ** -0.5, 0.125, ((0, 8), (1, 2)), jnp.float32),
        "glu_weight": scatter_about(key_of[5], (D, D), D ** -0.5, 0.125, ((0, 8), (1, 2)), jnp.float32),
        "out_weight": scatter_about(key_of[6], (D, D), D ** -0.5, 0.125, ((0, 8), (1, 2)), jnp.float32),
        "gate_scale": jnp.clip(1.0 + 0.18 * jax.random.normal(key_of[7], (FF,), jnp.float32), 0.1, 1.9),
        "up_scale": jnp.clip(jnp.exp(math.log(2.0) - 1.3862944 * jax.random.uniform(key_of[8], (FF,), jnp.float32) ** shard_levels(key_of[8], (FF,), ((0, 2),), -0.2, 0.2)), 0.5, 2.0),
        "down_scale": jnp.clip(jnp.exp(math.log(4.0) - 1.3862944 * jax.random.uniform(key_of[9], (D,), jnp.float32) ** shard_levels(key_of[9], (D,), ((0, 8),), -0.2, 0.2)), 1.0, 4.0),
        "value_scale": draw_value_scale(jax.random.fold_in(key_of[18], 71), 0),
        "glu_scale": jnp.clip(1.0 + 0.18 * jax.random.normal(key_of[11], (D,), jnp.float32), 0.1, 1.9),
        "out_scale": jnp.clip(jnp.exp(math.log(4.0) - 1.3862944 * jax.random.uniform(key_of[12], (D,), jnp.float32) ** shard_levels(key_of[12], (D,), ((0, 8),), -0.2, 0.2)), 1.0, 4.0),
        "conv_kernel": scatter_about(key_of[13], (KW, D), KW ** -0.5, 1.0, ((1, 2),), jnp.float32),
        "norm_gain": jnp.clip(1.0 + 0.18 * jax.random.normal(key_of[14], (D,), jnp.float32), 0.1, 1.9),
        "first_gain": jnp.clip(1.0 + 0.18 * jax.random.normal(key_of[15], (D,), jnp.float32), 0.1, 1.9),
        "conv_gain": jnp.clip(1.0 + 0.18 * jax.random.normal(key_of[16], (D,), jnp.float32), 0.1, 1.9),
        "second_gain": jnp.clip(1.0 + 0.18 * jax.random.normal(key_of[17], (D,), jnp.float32), 0.1, 1.9),
    }


EPSILON = 1e-06

def rms_rows(rows, gains):
    values = rows.astype(jnp.float32)
    scaled = values * lax.rsqrt(lax.optimization_barrier(jnp.mean(values * values, axis=-1, keepdims=True)) + EPSILON)
    return (scaled * gains).astype(jnp.bfloat16)

def gated_hidden(normed, gate_full, up_full, gate_scale, up_scale):
    gate_part = jnp.dot(normed, gate_full, preferred_element_type=jnp.float32) * gate_scale
    upward = jnp.dot(normed, up_full, preferred_element_type=jnp.float32) * up_scale
    return (jax.nn.silu(gate_part) * upward).astype(jnp.bfloat16)

def block_sum(active, weight_rows):
    width = active.shape[1] // N_TP
    total = jnp.zeros((active.shape[0], weight_rows.shape[0]), jnp.float32)
    for block in range(N_TP):
        partial_term = lax.dot_general(active[:, block * width:(block + 1) * width], weight_rows[:, block * width:(block + 1) * width], (((1,), (1,)), ((), ())), preferred_element_type=jnp.float32)
        rounded = lax.optimization_barrier(partial_term.astype(jnp.bfloat16))
        total = total + rounded.astype(jnp.float32)
    return total

def causal_depthwise(inputs, kernel):
    taps = kernel.shape[0]
    length = inputs.shape[0]
    padded = jnp.concatenate([jnp.zeros((taps - 1, inputs.shape[1]), jnp.float32), inputs.astype(jnp.float32)], axis=0)
    total = jnp.zeros((length, inputs.shape[1]), jnp.float32)
    for offset in range(taps):
        total = total + kernel[offset] * padded[offset:offset + length]
    return total

def reference(tokens, gate_weight, up_weight, down_weight, value_weight, glu_weight, out_weight, gate_scale, up_scale, down_scale, value_scale, glu_scale, out_scale, conv_kernel, norm_gain, first_gain, conv_gain, second_gain):
    gate_full = gate_weight.astype(jnp.bfloat16)
    up_full = up_weight.astype(jnp.bfloat16)
    down_full = down_weight.astype(jnp.bfloat16)
    value_full = value_weight.astype(jnp.bfloat16)
    glu_full = glu_weight.astype(jnp.bfloat16)
    out_full = out_weight.astype(jnp.bfloat16)

    def one_sequence(rows):
        hidden = gated_hidden(rms_rows(rows, first_gain), gate_full, up_full, gate_scale, up_scale)
        after_first = (rows.astype(jnp.float32) + 0.5 * down_scale * block_sum(hidden, down_full)).astype(jnp.bfloat16)
        normed = rms_rows(after_first, conv_gain)
        value_part = jnp.dot(normed, value_full, preferred_element_type=jnp.float32) * value_scale
        gate_part = jnp.dot(normed, glu_full, preferred_element_type=jnp.float32) * glu_scale
        glu_in = (value_part * jax.nn.sigmoid(gate_part)).astype(jnp.bfloat16)
        mixed = causal_depthwise(glu_in, conv_kernel)
        mean_rows = lax.optimization_barrier(jnp.mean(mixed, axis=1, keepdims=True))
        square_rows = lax.optimization_barrier(jnp.mean(mixed * mixed, axis=1, keepdims=True))
        normalized = (mixed - mean_rows) * lax.rsqrt(square_rows - mean_rows * mean_rows + EPSILON) * norm_gain
        active = jax.nn.silu(normalized).astype(jnp.bfloat16)
        after_conv = (after_first.astype(jnp.float32) + out_scale * block_sum(active, out_full)).astype(jnp.bfloat16)
        hidden = gated_hidden(rms_rows(after_conv, second_gain), gate_full, up_full, gate_scale, up_scale)
        return (after_conv.astype(jnp.float32) + 0.5 * down_scale * block_sum(hidden, down_full)).astype(jnp.bfloat16)
    groups = tokens.reshape(N_REP * N_FS, SEQ, D)
    return lax.map(one_sequence, groups).reshape(TOKENS, D)
```

```python
import jax
import jax.numpy as jnp
from jax import lax
from jax.sharding import PartitionSpec as P

D = 2048


EPSILON = 1e-06


def rms_rows(rows, gains):
    values = rows.astype(jnp.float32)
    scaled = values * lax.rsqrt(jnp.mean(values * values, axis=-1, keepdims=True) + EPSILON)
    return (scaled * gains).astype(jnp.bfloat16)


def gated_hidden(normed, gate_full, up_full, gate_scale, up_scale):
    gate_part = jnp.dot(normed, gate_full, preferred_element_type=jnp.float32) * gate_scale
    upward = jnp.dot(normed, up_full, preferred_element_type=jnp.float32) * up_scale
    return (jax.nn.silu(gate_part) * upward).astype(jnp.bfloat16)


def causal_depthwise(inputs, kernel):
    taps = kernel.shape[0]
    length = inputs.shape[0]
    padded = jnp.concatenate(
        [jnp.zeros((taps - 1, inputs.shape[1]), jnp.float32), inputs.astype(jnp.float32)], axis=0
    )
    total = jnp.zeros((length, inputs.shape[1]), jnp.float32)
    for offset in range(taps):
        total = total + kernel[offset] * padded[offset : offset + length]
    return total


def swap(values, axis):
    return lax.ppermute(values, axis, [(0, 1), (1, 0)])


def gather_rows(rows, axis):
    if lax.axis_size(axis) != 2:
        return lax.all_gather(rows, axis, axis=0, tiled=True)
    other = swap(rows, axis)
    first = lax.axis_index(axis) == 0
    return jnp.concatenate([jnp.where(first, rows, other), jnp.where(first, other, rows)], axis=0)


def scatter_rows(partial, axis):
    members = lax.axis_size(axis)
    if members != 2:
        return lax.psum_scatter(partial, axis, scatter_dimension=0, tiled=True).astype(jnp.float32)
    own_rows = partial.shape[0] // members
    place = lax.axis_index(axis)
    mine = lax.dynamic_slice_in_dim(partial, place * own_rows, own_rows, 0)
    theirs = lax.dynamic_slice_in_dim(partial, (1 - place) * own_rows, own_rows, 0)
    return mine.astype(jnp.float32) + swap(theirs, axis).astype(jnp.float32)


def pull(rows, step):
    n = lax.axis_size("rep")
    return lax.ppermute(rows, "rep", [(s, (s - step) % n) for s in range(n)])


def push(rows, step):
    n = lax.axis_size("rep")
    return lax.ppermute(rows, "rep", [(s, (s + step) % n) for s in range(n)])


def streams_of(own):
    n = lax.axis_size("rep")
    parts = [own] + [pull(own, step) for step in range(1, n)]
    return [gather_rows(part, "tp") for part in parts]


def owned_sum(actives, weight_rows):
    n = lax.axis_size("rep")
    total = None
    for step in list(range(1, n)) + [0]:
        partial = lax.dot_general(
            actives[step], weight_rows, (((1,), (1,)), ((), ())), preferred_element_type=jnp.float32
        ).astype(jnp.bfloat16)
        part = scatter_rows(partial, "tp")
        if step:
            part = push(part.astype(jnp.bfloat16), step).astype(jnp.float32)
        total = part if total is None else total + part
    return total


def local(
    tokens,
    gate_weight,
    up_weight,
    down_weight,
    value_weight,
    glu_weight,
    out_weight,
    gate_scale,
    up_scale,
    down_scale,
    value_scale,
    glu_scale,
    out_scale,
    conv_kernel,
    norm_gain,
    first_gain,
    conv_gain,
    second_gain,
):
    reps = lax.axis_size("rep")
    rep = lax.axis_index("rep")

    def part(array, dim):
        width = array.shape[dim] // reps
        return lax.dynamic_slice_in_dim(array, rep * width, width, dim)

    scales = lax.all_gather(jnp.stack([down_scale, out_scale]), "fs", axis=1, tiled=True)
    down_rows, out_rows = scales[0], scales[1]

    def full(weight):
        return lax.all_gather(part(weight, 1).astype(jnp.bfloat16), "fs", axis=0, tiled=True)

    gate_full, up_full, down_full, value_full, glu_full, out_full = (
        full(gate_weight),
        full(up_weight),
        full(down_weight),
        full(value_weight),
        full(glu_weight),
        full(out_weight),
    )
    gate_scale, up_scale, value_scale, glu_scale, norm_gain = (
        part(gate_scale, 0),
        part(up_scale, 0),
        part(value_scale, 0),
        part(glu_scale, 0),
        part(norm_gain, 0),
    )
    conv_kernel = part(conv_kernel, 1)
    members = lax.axis_size("tp")
    own_rows = tokens.shape[0] // members
    own_tokens = lax.dynamic_slice_in_dim(tokens, lax.axis_index("tp") * own_rows, own_rows, 0)

    normed = rms_rows(tokens, first_gain)
    own_normed = rms_rows(own_tokens, first_gain)
    rows = [normed] + [gather_rows(pull(own_normed, step), "tp") for step in range(1, reps)]
    hidden = [gated_hidden(r, gate_full, up_full, gate_scale, up_scale) for r in rows]
    after_first = (
        own_tokens.astype(jnp.float32) + 0.5 * down_rows * owned_sum(hidden, down_full)
    ).astype(jnp.bfloat16)
    mixes, sums = [], []
    for rows in streams_of(rms_rows(after_first, conv_gain)):
        value_part = jnp.dot(rows, value_full, preferred_element_type=jnp.float32) * value_scale
        gate_part = jnp.dot(rows, glu_full, preferred_element_type=jnp.float32) * glu_scale
        glu_in = (value_part * jax.nn.sigmoid(gate_part)).astype(jnp.bfloat16)
        mixed = causal_depthwise(glu_in, conv_kernel)
        mixes.append(mixed)
        sums.append(jnp.stack([jnp.sum(mixed, axis=1), jnp.sum(mixed * mixed, axis=1)]))
    totals = lax.psum(jnp.roll(jnp.stack(sums), rep, axis=0), ("rep", "tp"))
    totals = jnp.roll(totals, -rep, axis=0) / D
    actives = []
    for step, mixed in enumerate(mixes):
        mean_rows = totals[step, 0][:, None]
        square_rows = totals[step, 1][:, None]
        normalized = (
            (mixed - mean_rows) * lax.rsqrt(square_rows - mean_rows * mean_rows + EPSILON) * norm_gain
        )
        actives.append(jax.nn.silu(normalized).astype(jnp.bfloat16))
    after_conv = (after_first.astype(jnp.float32) + out_rows * owned_sum(actives, out_full)).astype(
        jnp.bfloat16
    )
    hidden = [
        gated_hidden(r, gate_full, up_full, gate_scale, up_scale)
        for r in streams_of(rms_rows(after_conv, second_gain))
    ]
    after_second = (
        after_conv.astype(jnp.float32) + 0.5 * down_rows * owned_sum(hidden, down_full)
    ).astype(jnp.bfloat16)
    return gather_rows(after_second, "tp")


def solution(mesh):
    placed = (
        P(("rep", "fs"), None),
        P("fs", "tp"),
        P("fs", "tp"),
        P("fs", "tp"),
        P("fs", "tp"),
        P("fs", "tp"),
        P("fs", "tp"),
        P("tp"),
        P("tp"),
        P("fs"),
        P("tp"),
        P("tp"),
        P("fs"),
        P(None, "tp"),
        P("tp"),
        P(),
        P(),
        P(),
    )
    return jax.shard_map(
        local, mesh=mesh, in_specs=placed, out_specs=P(("rep", "fs"), None), check_vma=False
    )
```
